32 devices in a mesh: ep: 4 (over y, x), tp: 8 (over z, core).
Axes of the slice: x: 2, y: 2, z: 4, core: 2. Of those that a mesh axis runs over, the one named last changes fastest.
Arguments:
- queries: bfloat16 [4096, 1024], P('ep', 'tp'), may hold values from -600 to 600
- key_rows: bfloat16 [4096, 128], P('ep'), may hold values from -6 to 6
- value_rows: bfloat16 [4096, 128], P('ep'), may hold values from -48 to 48
- sink_logits: float32 [16], P('tp'), may hold values from 2 to 6
- out_weight: bfloat16 [1024, 2048], P('tp'), may hold values from -0.1875 to 0.1875
- moe_rows: bfloat16 [1024, 2048], P(('ep', 'tp')), may hold values from -6 to 6
- moe_gain: float32 [2048], replicated, may hold values from 0.1 to 1.9
- routes: int32 [1024, 2], P(('ep', 'tp')), may hold values from 0 to 3, all different within a row; in each aligned block of 32 rows (0 to 31, 32 to 63, ...) at most 24 rows name the same one
- route_weight: float32 [1024, 2], P(('ep', 'tp')), may hold values from 0.2 to 1
- gate_weight: bfloat16 [4, 2048, 7168], P('ep', None, 'tp'), may hold values from -0.125 to 0.125
- up_weight: bfloat16 [4, 2048, 7168], P('ep', None, 'tp'), may hold values from -0.125 to 0.125
- down_weight: bfloat16 [4, 7168, 2048], P('ep', 'tp'), may hold values from -0.0625 to 0.0625
Outputs:
- mixer_out: bfloat16 [4096, 2048], P(('ep', 'tp'))
- moe_out: bfloat16 [1024, 2048], P(('ep', 'tp'))
The draws below stay inside these ranges and needn't reach their ends.
Inputs may be any that keep to these rules, and one draw needn't show every extreme that they name: `routes`: in each aligned block of 32 rows (the rows of one device) no expert is named more than 24 times, a bound that some block reaches; each row names 2 different experts.
All inputs are finite; a program needn't handle non-finite values.
Results may differ from the reference program's by a relative error of at most 0.02.
Values may be sent and summed in bfloat16 or wider, within the bound.
A program may use at most 128 MiB of HBM per device.

```python
import math
import jax
import jax.numpy as jnp
import numpy as np
from jax import lax

D = 2048
HEADS = 16
KV_HEADS = 2
HEAD_DIM = 64
WINDOW = 128
FF = 7168
TOP = 2
MOE_DEV = 32
EXPERTS = 4
TOKENS = 4096
MOE_TOKENS = 1024
CAP = 24
N_TP = 8


def draw_queries(key, part):
    base = jax.random.truncated_normal(key, -6.0, 6.0, (TOKENS, HEADS * HEAD_DIM), jnp.float32)
    return base.astype(jnp.bfloat16)


def block_levels(rng, extent, shards, smallest, largest):
    level, own = 1.0, jax.random.fold_in(rng, 6)
    for dim, shards_of in shards:
        draws = jnp.exp(jax.random.uniform(jax.random.fold_in(own, dim), (shards_of,), jnp.float32, smallest / len(shards), largest / len(shards)))
        level = level * jnp.repeat(draws, extent[dim] // shards_of).reshape([-1 if axis == dim else 1 for axis in range(len(extent))])
    return level


def assign_block(own_key, own, number, rows, count, top, most, slope):
    sequence = jax.random.permutation(own_key, count)
    crowded, ordinary = portions_of(count, rows * top, most, slope, True), portions_of(count, rows * top, most, slope, False)
    places = jnp.arange(count)

    def named(tallies, turn):
        used = int((tallies > 0).sum())
        fixed = max(1, used // 4)
        shifted = fixed + (places - fixed + turn * (used - fixed)) % max(1, count - fixed)
        return jnp.zeros((count,), jnp.int32).at[sequence[jnp.where(places < fixed, places, shifted)]].set(jnp.asarray(tallies, jnp.int32))

    tallies = jnp.where(number % 4 == 0, named(crowded, number // 4), named(ordinary, number - number // 4 - 1))
    mixed = jax.random.permutation(jax.random.fold_in(own, 3), count)
    donor, receiver = mixed[0:count // 2 * 2:2], mixed[1:count // 2 * 2:2]
    room = jnp.minimum(tallies[donor] - 1, most - tallies[receiver]) // 2
    room = jnp.where((donor == sequence[0]) | (receiver == sequence[0]) | (tallies[receiver] == 0), 0, jnp.maximum(room, 0))
    shifted = jax.random.randint(jax.random.fold_in(own, 4), (count // 2,), 0, 1 << 20) % (room + 1)
    tallies = tallies.at[donor].add(-shifted).at[receiver].add(shifted)
    members = jnp.searchsorted(jnp.cumsum(tallies), jnp.arange(rows * top), side="right").astype(jnp.int32)
    listing = members.reshape(top, rows).T
    listing = listing[jax.random.permutation(jax.random.fold_in(own, 1), rows)]
    turn = jax.random.randint(jax.random.fold_in(own, 2), (rows, 1), 0, top)
    return jnp.take_along_axis(listing, (jnp.arange(top)[None, :] + turn) % top, axis=1)


def portions_of(amount, total, most, slope, full):
    loads = [(1 << 20) // math.isqrt(standing ** slope) + 1 for standing in range(1, amount + 1)]
    largest = most if full else min(most, max(-(-total // amount), total * loads[0] // sum(loads)))
    least = 1 if total - largest >= amount - 1 else 0
    given, rest = [largest] + [least] * (amount - 1), total - largest - least * (amount - 1)
    while rest > 0:
        free = [i for i in range(1, amount) if given[i] < largest] or [i for i in range(1, amount) if given[i] < most]
        mass, budget = sum([loads[i] for i in free]), rest
        for i in free:
            more = min(most - given[i], max(1, budget * loads[i] // mass), rest)
            given[i] = given[i] + more
            rest = rest - more
    return np.array(given)


def centred(rng, dims, scale, bound, shards=(), kind=jnp.bfloat16):
    level = block_levels(rng, dims, shards, -0.22, 0.18) if shards else 1.0
    drawn = jax.random.normal(rng, dims, jnp.float32) * scale * level
    return jnp.minimum(jnp.maximum(drawn, -bound), bound).astype(kind)


def setup_inputs(seed: int = 0) -> dict:
    seeds = jax.random.split(jax.random.key(seed), 13)
    queries = draw_queries(jax.random.fold_in(seeds[12], 71), 0)
    key_rows = centred(seeds[1], (TOKENS, KV_HEADS * HEAD_DIM), 1.0, 6.0, ((0, 4),))
    value_rows = centred(seeds[2], (TOKENS, KV_HEADS * HEAD_DIM), 8.0, 48.0, ((0, 4),))
    sink_logits = jnp.clip(2.0 + 4.0 * jax.random.uniform(seeds[3], (HEADS,), jnp.float32) ** block_levels(seeds[3], (HEADS,), ((0, 8),), -0.2, 0.2), 2.0, 6.0)
    out_weight = centred(seeds[4], (HEADS * HEAD_DIM, D), (HEADS * HEAD_DIM) ** -0.5, 0.1875, ((0, 8),))
    moe_rows = centred(seeds[5], (MOE_TOKENS, D), 1.0, 6.0, ((0, 32),))
    moe_gain = jnp.clip(1.0 + 0.18 * jax.random.normal(seeds[6], (D,), jnp.float32), 0.1, 1.9)
    routes_keys = jax.random.split(jax.random.fold_in(seeds[7], 1), MOE_TOKENS // MOE_DEV)
    routes_turns = jax.random.permutation(jax.random.fold_in(seeds[7], 3), MOE_TOKENS // MOE_DEV)
    routes = jax.vmap(lambda own, number: assign_block(jax.random.fold_in(seeds[7], 2), own, number, MOE_DEV, EXPERTS, TOP, CAP, 2))(routes_keys, routes_turns).reshape((MOE_TOKENS, TOP))
    route_weight = jnp.clip(0.2 + 0.8 * jax.random.uniform(seeds[8], (MOE_TOKENS, TOP), jnp.float32) ** block_levels(seeds[8], (MOE_TOKENS, TOP), ((0, 32),), -0.2, 0.2), 0.2, 1.0)
    gate_weight = centred(seeds[9], (EXPERTS, D, FF), D ** -0.5, 0.125, ((0, 4), (2, 8)))
    up_weight = centred(seeds[10], (EXPERTS, D, FF), D ** -0.5, 0.125, ((0, 4), (2, 8)))
    down_weight = centred(seeds[11], (EXPERTS, FF, D), FF ** -0.5, 0.0625, ((0, 4), (1, 8)))
    return {"queries": queries, "key_rows": key_rows, "value_rows": value_rows, "sink_logits": sink_logits, "out_weight": out_weight, "moe_rows": moe_rows, "moe_gain": moe_gain, "routes": routes, "route_weight": route_weight, "gate_weight": gate_weight, "up_weight": up_weight, "down_weight": down_weight}


big_negative = -1e+30
norm_eps = 1e-05

def stored_bf16(values):
    return lax.optimization_barrier(values.astype(jnp.bfloat16)).astype(jnp.float32)

def layer_normed(inputs, gain):
    values = inputs.astype(jnp.float32)
    center = values - lax.optimization_barrier(jnp.mean(values, -1, keepdims=True))
    spread = lax.optimization_barrier(jnp.mean(center * center, -1, keepdims=True))
    return (center * lax.rsqrt(spread + norm_eps) * gain).astype(jnp.bfloat16)

def one_head(head_index, queries, key_rows, value_rows, sink_logits):
    total = queries.shape[0]
    blocks = total // WINDOW
    key_head = head_index // (HEADS // KV_HEADS)
    query_cols = lax.dynamic_slice_in_dim(queries, head_index * HEAD_DIM, HEAD_DIM, 1).astype(jnp.float32)
    key_cols = lax.dynamic_slice_in_dim(key_rows, key_head * HEAD_DIM, HEAD_DIM, 1).astype(jnp.float32)
    value_cols = lax.dynamic_slice_in_dim(value_rows, key_head * HEAD_DIM, HEAD_DIM, 1).astype(jnp.float32)
    padding = jnp.zeros((WINDOW, HEAD_DIM), jnp.float32)
    key_ext = jnp.concatenate([padding, key_cols], 0)
    value_ext = jnp.concatenate([padding, value_cols], 0)
    key_blocks = jnp.concatenate([key_ext[:total].reshape(blocks, WINDOW, HEAD_DIM), key_ext[WINDOW:].reshape(blocks, WINDOW, HEAD_DIM)], 1)
    value_blocks = jnp.concatenate([value_ext[:total].reshape(blocks, WINDOW, HEAD_DIM), value_ext[WINDOW:].reshape(blocks, WINDOW, HEAD_DIM)], 1)
    scores = jnp.einsum('nqd,nkd->nqk', query_cols.reshape(blocks, WINDOW, HEAD_DIM), key_blocks) * HEAD_DIM ** (-0.5)
    block_base = jnp.arange(blocks, dtype=jnp.int32)[:, None, None] * WINDOW
    query_pos = block_base + jnp.arange(WINDOW, dtype=jnp.int32)[None, :, None]
    key_pos = block_base - WINDOW + jnp.arange(2 * WINDOW, dtype=jnp.int32)[None, None, :]
    allowed = (key_pos <= query_pos) & (key_pos > query_pos - WINDOW) & (key_pos >= 0)
    masked = jnp.where(allowed, scores, big_negative)
    sink = sink_logits[head_index]
    row_max = jnp.maximum(lax.optimization_barrier(jnp.max(masked, -1)), sink)
    powers = jnp.where(allowed, jnp.exp(masked - row_max[..., None]), 0.0)
    totals = lax.optimization_barrier(jnp.sum(powers, -1)) + jnp.exp(sink - row_max)
    attn_probs = stored_bf16(powers / totals[..., None])
    attended = jnp.einsum('nqk,nkd->nqd', attn_probs, value_blocks)
    return attended.astype(jnp.bfloat16).reshape(total, HEAD_DIM)

def one_expert(inputs):
    expert_rows, gate_mat, up_mat, down_mat = inputs
    gate_val = jnp.dot(expert_rows, gate_mat, preferred_element_type=jnp.float32)
    up_val = jnp.dot(expert_rows, up_mat, preferred_element_type=jnp.float32)
    hidden = (jax.nn.silu(gate_val) * up_val).astype(jnp.bfloat16)
    group_units = FF // N_TP

    def add_group(index, carry):
        first_col = index.astype(jnp.int32) * group_units
        hidden_cols = lax.dynamic_slice_in_dim(hidden, first_col, group_units, 1)
        down_rows = lax.dynamic_slice_in_dim(down_mat, first_col, group_units, 0)
        return carry + stored_bf16(jnp.dot(hidden_cols, down_rows, preferred_element_type=jnp.float32))
    summed = lax.fori_loop(0, N_TP, add_group, jnp.zeros((expert_rows.shape[0], D), jnp.float32))
    return summed.astype(jnp.bfloat16)

def reference(queries, key_rows, value_rows, sink_logits, out_weight, moe_rows, moe_gain, routes, route_weight, gate_weight, up_weight, down_weight):
    total = queries.shape[0]
    per_head = lax.map(lambda index: one_head(index, queries, key_rows, value_rows, sink_logits), jnp.arange(HEADS, dtype=jnp.int32))
    attended = jnp.transpose(per_head, (1, 0, 2)).reshape(total, HEADS * HEAD_DIM)
    group_cols = HEADS // N_TP * HEAD_DIM

    def add_heads(index, carry):
        first_col = index.astype(jnp.int32) * group_cols
        head_cols = lax.dynamic_slice_in_dim(attended, first_col, group_cols, 1)
        proj_rows = lax.dynamic_slice_in_dim(out_weight, first_col, group_cols, 0)
        return carry + stored_bf16(jnp.dot(head_cols, proj_rows, preferred_element_type=jnp.float32))
    mixer_out = lax.fori_loop(0, N_TP, add_heads, jnp.zeros((total, D), jnp.float32)).astype(jnp.bfloat16)
    normed = layer_normed(moe_rows, moe_gain)
    devices = MOE_TOKENS // MOE_DEV
    chosen = routes.reshape(devices, MOE_DEV * TOP).astype(jnp.int32)
    onehot = (chosen[..., None] == jnp.arange(EXPERTS, dtype=jnp.int32)[None, None, :]).astype(jnp.int32)
    earlier_count = jnp.cumsum(onehot, 1) - onehot
    slot_index = lax.optimization_barrier(jnp.sum(earlier_count * onehot, -1)).astype(jnp.int32)
    device_index = jnp.arange(devices, dtype=jnp.int32)[:, None]
    position = ((chosen * devices + device_index) * CAP + slot_index).reshape(-1).astype(jnp.int32)
    token_of = (jnp.arange(MOE_TOKENS * TOP, dtype=jnp.int32) // TOP).astype(jnp.int32)
    buffer = jnp.zeros((EXPERTS * devices * CAP, D), jnp.bfloat16).at[position].set(normed[token_of])
    buffer = buffer.reshape(EXPERTS, devices * CAP, D)
    results = lax.map(one_expert, (buffer, gate_weight, up_weight, down_weight))
    picked = results.reshape(EXPERTS * devices * CAP, D)[position].astype(jnp.float32)
    picked = picked.reshape(MOE_TOKENS, TOP, D)
    moe_out = lax.optimization_barrier(jnp.sum(picked * route_weight[:, :, None], 1)).astype(jnp.bfloat16)
    return (mixer_out, moe_out)
```

```python
import functools

import jax
import jax.numpy as jnp
from jax import lax
from jax.experimental import pallas as pl
from jax.experimental.pallas import tpu as pltpu
from jax.sharding import PartitionSpec as P

MESH = pl.DeviceIdType.MESH

HEADS = 16
KV_HEADS = 2
HEAD_DIM = 64
WINDOW = 128
TOP = 2


big_negative = -1e30
norm_eps = 1e-05


def passed_along(value, axis, steps):
    count = lax.axis_size(axis)
    initial, last = (max(0, -steps), min(count, count - steps))
    return lax.ppermute(value, axis, [(source, source + steps) for source in range(initial, last)])


def layer_normed(inputs, gain):
    values = inputs.astype(jnp.float32)
    center = values - jnp.mean(values, -1, keepdims=True)
    spread = jnp.mean(center * center, -1, keepdims=True)
    return (center * lax.rsqrt(spread + norm_eps) * gain).astype(jnp.bfloat16)


def attend(queries, key_rows, value_rows, sink_logits):
    total = queries.shape[0]
    heads_here = sink_logits.shape[0]
    blocks = total // WINDOW
    key_head = lax.axis_index("tp") * heads_here // (HEADS // KV_HEADS)
    key_own = lax.dynamic_slice_in_dim(key_rows, key_head * HEAD_DIM, HEAD_DIM, 1)
    value_own = lax.dynamic_slice_in_dim(value_rows, key_head * HEAD_DIM, HEAD_DIM, 1)
    last_rows = jnp.concatenate([key_own[total - WINDOW :], value_own[total - WINDOW :]], 1)
    earlier = passed_along(last_rows, "ep", 1)
    key_ext = jnp.concatenate([earlier[:, :HEAD_DIM], key_own], 0)
    value_ext = jnp.concatenate([earlier[:, HEAD_DIM:], value_own], 0)
    key_blocks = jnp.concatenate(
        [
            key_ext[:total].reshape(blocks, WINDOW, HEAD_DIM),
            key_ext[WINDOW:].reshape(blocks, WINDOW, HEAD_DIM),
        ],
        1,
    )
    value_blocks = jnp.concatenate(
        [
            value_ext[:total].reshape(blocks, WINDOW, HEAD_DIM),
            value_ext[WINDOW:].reshape(blocks, WINDOW, HEAD_DIM),
        ],
        1,
    )
    query_blocks = queries.reshape(blocks, WINDOW, heads_here, HEAD_DIM)
    scores = jnp.einsum(
        "nqhd,nkd->nhqk", query_blocks, key_blocks, preferred_element_type=jnp.float32
    ) * HEAD_DIM ** (-0.5)
    anchor = lax.axis_index("ep") * total
    block_base = anchor + jnp.arange(blocks, dtype=jnp.int32)[:, None, None] * WINDOW
    query_pos = block_base + jnp.arange(WINDOW, dtype=jnp.int32)[None, :, None]
    key_pos = block_base - WINDOW + jnp.arange(2 * WINDOW, dtype=jnp.int32)[None, None, :]
    allowed = ((key_pos <= query_pos) & (key_pos > query_pos - WINDOW) & (key_pos >= 0))[:, None]
    masked = jnp.where(allowed, scores, big_negative)
    sinks = sink_logits[None, :, None]
    row_max = jnp.maximum(jnp.max(masked, -1), sinks)
    powers = jnp.where(allowed, jnp.exp(masked - row_max[..., None]), 0.0)
    totals = jnp.sum(powers, -1) + jnp.exp(sinks - row_max)
    attn_probs = (powers / totals[..., None]).astype(jnp.bfloat16)
    attended = jnp.einsum(
        "nhqk,nkd->nqhd", attn_probs, value_blocks, preferred_element_type=jnp.float32
    )
    return attended.astype(jnp.bfloat16).reshape(total, heads_here * HEAD_DIM)


def mixer(queries, key_rows, value_rows, sink_logits, out_weight):
    attended = attend(queries, key_rows, value_rows, sink_logits)
    return lax.psum_scatter(
        jnp.dot(attended, out_weight, preferred_element_type=jnp.float32).astype(jnp.bfloat16),
        "tp",
        scatter_dimension=0,
        tiled=True,
    )


def experts(moe_rows, moe_gain, routes, route_weight, gate_weight, up_weight, down_weight):
    row_count = moe_rows.shape[0]
    width_all = moe_rows.shape[1]
    expert_count = gate_weight.shape[0] * lax.axis_size("ep")
    capacity = 3 * row_count * TOP // (2 * expert_count)
    normed = layer_normed(moe_rows, moe_gain)
    chosen = routes.reshape(-1)
    onehot = (chosen[:, None] == jnp.arange(expert_count, dtype=jnp.int32)[None, :]).astype(
        jnp.int32
    )
    earlier_count = jnp.cumsum(onehot, 0) - onehot
    slot_index = jnp.sum(earlier_count * onehot, 1)
    target = chosen * capacity + slot_index
    matches = target[None, :] == jnp.arange(expert_count * capacity, dtype=jnp.int32)[:, None]
    dispatch_map = jnp.sum(matches.reshape(expert_count * capacity, row_count, TOP), -1).astype(
        jnp.bfloat16
    )
    buffer = jnp.dot(dispatch_map, normed, preferred_element_type=jnp.float32).astype(jnp.bfloat16)
    buffer = buffer.reshape(expert_count, capacity, width_all)
    gate_mat = gate_weight[0]
    up_mat = up_weight[0]
    down_mat = down_weight[0]
    received = lax.all_to_all(buffer, "ep", split_axis=0, concat_axis=0, tiled=True)
    total = received.shape[0] * received.shape[1]
    flat_rows = received.reshape(total, width_all)
    shard_rows = lax.all_gather(flat_rows, "tp", axis=0, tiled=True)
    gate_val = jnp.dot(shard_rows, gate_mat, preferred_element_type=jnp.float32)
    up_val = jnp.dot(shard_rows, up_mat, preferred_element_type=jnp.float32)
    hidden = (jax.nn.silu(gate_val) * up_val).astype(jnp.bfloat16)
    summed = lax.psum_scatter(
        jnp.dot(hidden, down_mat, preferred_element_type=jnp.float32).astype(jnp.bfloat16),
        "tp",
        scatter_dimension=0,
        tiled=True,
    )
    results = summed.reshape(received.shape)
    returned = lax.all_to_all(results, "ep", split_axis=0, concat_axis=0, tiled=True)
    weights_flat = route_weight.reshape(-1)
    combine_map = jnp.sum(
        jnp.where(matches, weights_flat[None, :], 0.0).reshape(
            expert_count * capacity, row_count, TOP
        ),
        -1,
    )
    returned_flat = returned.reshape(expert_count * capacity, width_all).astype(jnp.float32)
    moe_out = lax.dot_general(
        combine_map, returned_flat, (((0,), (0,)), ((), ())), precision=lax.Precision.HIGHEST
    )
    return moe_out.astype(jnp.bfloat16)


def fused_kernel(
    groups,
    ranks,
    chosen_ref,
    weights_ref,
    sink_ref,
    rows_ref,
    gain_ref,
    q_hbm,
    key_hbm,
    value_hbm,
    ow_hbm,
    gate_hbm,
    up_hbm,
    down_hbm,
    mix_hbm,
    moe_hbm,
    x_buf,
    p_buf,
    r1_buf,
    r2_buf,
    r3_buf,
    rc_buf,
    w_buf,
    qb_buf,
    l_buf,
    halo,
    kdup,
    vdup,
    att,
    hid,
    mix_v,
    q_ref,
    key_ref,
    value_ref,
    gate_w,
    up_w,
    down_w,
    load_sem,
    out_sem,
    sem,
    z_rs,
    x1_rs,
    x2_rs,
    pa_rs,
    zl_rs,
    l1_rs,
    l2_rs,
    lp_rs,
    w_rs,
    wp_rs,
    wx_rs,
    wq_rs,
    s1_rs,
    s2_rs,
    s3_rs,
    rc_rs,
    q_rs,
    halo_rs,
):
    chips = ranks // 2
    e, t = lax.axis_index("ep"), lax.axis_index("tp")
    z, c = lax.div(t, 2), lax.rem(t, 2)
    y, x = lax.div(e, 2), lax.rem(e, 2)
    me = e * ranks + t
    ex, ey, e3 = e + 1 - 2 * x, e + 2 - 4 * y, 3 - e
    e1 = ex * (1 - c) + ey * c
    e2 = ey * (1 - c) + ex * c
    other = t + 1 - 2 * c
    oc = 1 - c
    mid = (z > 0) & (z < chips - 1)
    edge = jnp.logical_not(mid)
    row_count, width = rows_ref.shape
    half_rows = row_count // 2
    units = gate_w.shape[1]
    upper = lax.div(z, 2)
    order = (z, z + 1 - 2 * lax.rem(z, 2), 2 - upper, 3 * (1 - upper))

    def plane(i):
        if isinstance(i, int):
            return order[i]
        later = jnp.where(i == 2, order[2], order[3])
        return jnp.where(i == 0, order[0], jnp.where(i == 1, order[1], later))

    def from_above(zz):
        return jnp.where(zz > z, 1, 0)

    def remote(src, dst, ss, rs, to):
        return pltpu.make_async_remote_copy(
            src_ref=src, dst_ref=dst, send_sem=ss, recv_sem=rs, device_id=to, device_id_type=MESH
        )

    ss = [sem.at[k] for k in range(sem.shape[0])]
    (zo_ss, zf_ss, x1_ss, x2_ss, pa_ss, zlo_ss, zlf_ss, l1_ss, l2_ss, lp_ss) = ss[:10]
    (wo_ss, wf_ss, wp_ss, wx_ss, wq_ss, s1_ss, s2_ss, s3_ss, rc_ss, q_ss, halo_ss) = ss[10:]

    def received(dst, rs):
        remote(dst, dst, x1_ss, rs, (e, other)).wait_recv()

    def sent(src, send_sem):
        remote(src, src, send_sem, x1_rs.at[0], (e, other)).wait_send()

    loads = [
        pltpu.make_async_copy(ow_hbm, w_buf.at[t], load_sem.at[0]),
        pltpu.make_async_copy(key_hbm, key_ref, load_sem.at[1]),
        pltpu.make_async_copy(value_hbm, value_ref, load_sem.at[2]),
        pltpu.make_async_copy(q_hbm, q_ref, load_sem.at[3]),
        pltpu.make_async_copy(gate_hbm.at[0], gate_w, load_sem.at[4]),
        pltpu.make_async_copy(up_hbm.at[0], up_w, load_sem.at[5]),
        pltpu.make_async_copy(down_hbm.at[0], down_w, load_sem.at[6]),
    ]
    for load in loads:
        load.start()

    barrier = pltpu.get_barrier_semaphore()

    def greet(to):
        pl.semaphore_signal(barrier, inc=1, device_id=to, device_id_type=MESH)

    for to in ((e, other), (e1, t), (e2, t)):
        greet(to)

    @pl.when(z > 0)
    def _():
        greet((e, t - 2))

    @pl.when(z < chips - 1)
    def _():
        greet((e, t + 2))

    values = rows_ref[...].astype(jnp.float32)
    center = values - jnp.mean(values, -1, keepdims=True)
    spread_of = jnp.mean(center * center, -1, keepdims=True)
    x_buf[z, e, c] = (center * lax.rsqrt(spread_of + norm_eps) * gain_ref[...]).astype(jnp.bfloat16)
    lane = lax.broadcasted_iota(jnp.int32, (1, 128), 1)
    sinks = jnp.zeros((1, 128), jnp.float32)
    for i in range(2):
        sinks = jnp.where(lane == row_count + i, sink_ref[:, i : i + 1], sinks)
    chosen, weights = chosen_ref[...], weights_ref[...]
    for k in range(groups):
        named = jnp.where(chosen == k, weights, 0.0)
        l_buf[z, e, c, k] = sinks
        l_buf[z, e, c, k, :, 0:row_count] = jnp.sum(named, 0, keepdims=True)

    with jax.named_scope("barrier"):
        pl.semaphore_wait(barrier, jnp.where(mid, 5, 4))

    def half(block, h):
        return block.at[pl.ds(h * half_rows, half_rows), :]

    def pair_send(zz, column, x_sems, l_sems, to):
        for buf, (send_sem, recv_sem) in ((x_buf, x_sems), (l_buf, l_sems)):
            piece = buf.at[zz, column, c]
            remote(piece, piece, send_sem, recv_sem, to).start()

    def z_send(zz, to, h, send_sem, line_sem):
        part = half(x_buf.at[zz, e, c], h)
        remote(part, part, send_sem, z_rs.at[zz * 2 + h], to).start()
        if h == 1:
            line = l_buf.at[zz, e, c]
            remote(line, line, line_sem, zl_rs.at[zz], to).start()

    def spread(zz):
        pair_send(zz, e, (x1_ss, x1_rs.at[zz]), (l1_ss, l1_rs.at[zz]), (e1, t))
        pair_send(zz, e, (x2_ss, x2_rs.at[zz]), (l2_ss, l2_rs.at[zz]), (e2, t))
        pair_send(zz, e, (pa_ss, pa_rs.at[zz]), (lp_ss, lp_rs.at[zz]), (e, other))

    @jax.named_scope("arrive")
    def arrive(i):
        zz = plane(i)
        to = (e, t + 2 - 4 * from_above(zz))
        for h in range(2):
            received(half(x_buf.at[zz, e, c], h), z_rs.at[zz * 2 + h])
            if h == 1:
                received(l_buf.at[zz, e, c], zl_rs.at[zz])

            @pl.when(mid)
            def _():
                z_send(zz, to, h, zf_ss, zlf_ss)

        spread(zz)

    @jax.named_scope("from_first")
    def from_first(zz):
        received(x_buf.at[zz, e1, c], x1_rs.at[zz])
        received(l_buf.at[zz, e1, c], l1_rs.at[zz])
        slot = chips + zz
        pair_send(zz, e1, (x2_ss, x2_rs.at[slot]), (l2_ss, l2_rs.at[slot]), (e2, t))
        pair_send(zz, e1, (pa_ss, pa_rs.at[zz]), (lp_ss, lp_rs.at[zz]), (e, other))

    @jax.named_scope("from_second")
    def from_second(zz):
        for slot, column in ((0, e2), (1, e3)):
            where = slot * chips + zz
            received(x_buf.at[zz, column, c], x2_rs.at[where])
            received(l_buf.at[zz, column, c], l2_rs.at[where])
            pair_send(zz, column, (pa_ss, pa_rs.at[zz]), (lp_ss, lp_rs.at[zz]), (e, other))

    @jax.named_scope("from_partner")
    def from_partner(zz):
        received(x_buf.at[zz, :, oc], pa_rs.at[zz])
        received(l_buf.at[zz, :, oc], lp_rs.at[zz])

    third = w_buf.shape[1] // 4
    side = x * (1 - c) + y * c
    carried = pl.ds(pl.multiple_of(side * third, third), 3 * third)
    given = pl.ds(pl.multiple_of(3 * side * third, third), third)
    taken = pl.ds(pl.multiple_of(3 * (1 - side) * third, third), third)
    other_side = x * c + y * (1 - c)
    other_carried = pl.ds(pl.multiple_of(other_side * third, third), 3 * third)
    other_taken = pl.ds(pl.multiple_of(3 * (1 - other_side) * third, third), third)

    def w_send(zz, to, send_sem):
        block = w_buf.at[zz * 2 + c, carried, :]
        remote(block, block, send_sem, w_rs.at[zz], to).start()

    def w_partner(zz):
        block = w_buf.at[zz * 2 + c, carried, :]
        remote(block, block, wp_ss, wp_rs.at[0], (e, other)).start()

    def w_rest(zz):
        rest = w_buf.at[zz * 2 + c, taken, :]
        remote(rest, rest, wq_ss, wq_rs.at[0], (e, other)).start()

    @jax.named_scope("w_arrive")
    def w_arrive(i):
        zz = plane(i)
        received(w_buf.at[zz * 2 + c, carried, :], w_rs.at[zz])

        @pl.when(mid)
        def _():
            w_send(zz, (e, t + 2 - 4 * from_above(zz)), wf_ss)

        piece = w_buf.at[zz * 2 + c, given, :]
        remote(piece, piece, wx_ss, wx_rs.at[zz], (e1, t)).start()
        w_partner(zz)

    def q_send(zz):
        for core in range(2):
            tt = zz * 2 + core

            @pl.when(tt != t)
            def _():
                remote(
                    q_ref.at[pl.ds(pl.multiple_of(tt * WINDOW, WINDOW), WINDOW), :],
                    qb_buf.at[t],
                    q_ss,
                    q_rs.at[z],
                    (e, tt),
                ).start()

    for h in range(2):

        @pl.when(z < chips - 1)
        def _():
            z_send(z, (e, t + 2), h, zo_ss, zlo_ss)

        @pl.when(z > 0)
        def _():
            z_send(z, (e, t - 2), h, zo_ss, zlo_ss)

    spread(z)
    loads[0].wait()
    ahead = (e, t + 2 - 4 * from_above(plane(1)))

    @pl.when(edge)
    def _():
        w_send(z, (e, jnp.where(z == 0, t + 2, t - 2)), wo_ss)

    w_partner(z)
    w_rest(z)
    from_first(z)
    arrive(1)

    @pl.when(mid)
    def _():
        w_send(z, ahead, wo_ss)
        arrive(2)
        arrive(3)
        w_send(z, (e, t - 2 + 4 * from_above(plane(1))), wo_ss)

    from_second(z)
    from_partner(z)
    for load in loads[1:4]:
        load.wait()

    last = key_ref.shape[0] - WINDOW
    gives = (t == 0) & (e < groups - 1)
    takes = (t == 0) & (e > 0)
    for i, source in enumerate((key_ref, value_ref)):
        copy = remote(
            source.at[pl.ds(last, WINDOW), :],
            halo.at[i],
            halo_ss,
            halo_rs.at[0],
            (lax.rem(e + 1, groups), t),
        )
        pl.when(gives)(copy.start)

    q_send(z)
    for load in loads[4:6]:
        load.wait()

    diagonal = lax.broadcasted_iota(jnp.int32, (row_count, 128), 0) == lax.broadcasted_iota(
        jnp.int32, (row_count, 128), 1
    )
    cut = (-(-units // 256) + 1) // 2 * 256
    rows_in_plane = groups * 2 * row_count

    @jax.named_scope("gate_up")
    def gate_up(zz, begin, end):
        rows = x_buf[zz].reshape(rows_in_plane, width)
        gate_val = jnp.dot(rows, gate_w[:, begin:end], preferred_element_type=jnp.float32)
        up_val = jnp.dot(rows, up_w[:, begin:end], preferred_element_type=jnp.float32)
        hid[:, begin:end] = (gate_val / (1.0 + jnp.exp(-gate_val)) * up_val).astype(jnp.bfloat16)

    def add_in(block, extra):
        block[...] = (block[...].astype(jnp.float32) + extra[...].astype(jnp.float32)).astype(
            jnp.bfloat16
        )

    @jax.named_scope("fold")
    def fold(i):
        zz = plane(i)
        received(r1_buf.at[zz], s1_rs.at[zz])
        for n, column in enumerate((e3, e2, e1, e)):
            block = p_buf.at[zz, column, c]
            add_in(block, r1_buf.at[zz, column])
            if n < 2:
                place = (1 - n) * chips + zz
                remote(block, r2_buf.at[1 - n, zz], s2_ss, s2_rs.at[place], (e2, t)).start()

    @jax.named_scope("second")
    def second(i):
        zz = plane(i)
        received(r2_buf.at[1, zz], s2_rs.at[chips + zz])
        block = p_buf.at[zz, e1, c]
        add_in(block, r2_buf.at[1, zz])
        remote(block, r3_buf.at[zz], s3_ss, s3_rs.at[zz], (e1, t)).start()

    @jax.named_scope("third_sum")
    def third_sum(i):
        zz = plane(i)
        received(r2_buf.at[0, zz], s2_rs.at[zz])
        received(r3_buf.at[zz], s3_rs.at[zz])
        block = p_buf.at[zz, e, c]
        block[...] = (
            block[...].astype(jnp.float32)
            + r2_buf[0, zz].astype(jnp.float32)
            + r3_buf[zz].astype(jnp.float32)
        ).astype(jnp.bfloat16)

    @jax.named_scope("chain")
    def chain(i, passing):
        zz = plane(i)
        hops = 2 if passing and i == 3 else 1
        to = (e, t + hops * (4 * from_above(zz) - 2))
        slot = 2 if i == 1 else 3 if passing else i - 2
        for h in range(2):
            part = half(p_buf.at[zz, e, c], h)
            if passing:
                extra = half(rc_buf.at[i - 2], h)
                received(extra, rc_rs.at[(i - 2) * 2 + h])
                add_in(part, extra)
            remote(part, half(rc_buf.at[slot], h), rc_ss, rc_rs.at[slot * 2 + h], to).start()

    @pl.loop(0, groups)
    def _(i):
        zz = plane(i)

        @pl.when(i > 0)
        def _():
            from_second(zz)
            from_partner(zz)
            q_send(zz)

        gate_up(zz, 0, cut)

        @pl.when(i == 0)
        def _():
            from_first(plane(1))
            pl.when(edge)(functools.partial(arrive, 2))

        @pl.when(i == 1)
        def _():
            from_first(plane(2))

        @pl.when(i == 2)
        def _():
            fold(0)

        @pl.when(i == 3)
        def _():
            fold(2)
            second(0)

        gate_up(zz, cut, units)

        @pl.when(i == 0)
        def _():
            loads[6].wait()

        @pl.when(i == 1)
        def _():
            from_first(plane(3))

        @pl.when(i == 2)
        def _():
            fold(1)

        @pl.when(i == 3)
        def _():
            second(1)

        shares = []
        for column in range(groups):
            for core in range(2):
                line = l_buf[zz, column, core, e]
                shares.append(
                    jnp.sum(
                        jnp.where(diagonal, jnp.broadcast_to(line, (row_count, 128)), 0.0),
                        -1,
                        keepdims=True,
                    )
                )
        share = jnp.concatenate(shares, 0)
        with jax.named_scope("down"):
            down = jnp.dot(hid[...], down_w[...], preferred_element_type=jnp.float32)
            p_buf[zz] = (down * share).astype(jnp.bfloat16).reshape(groups, 2, row_count, width)
        remote(p_buf.at[zz, :, oc], r1_buf.at[zz], s1_ss, s1_rs.at[zz], (e, other)).start()

        @pl.when((i == 0) & edge)
        def _():
            arrive(3)

        @pl.when((i == 1) & mid)
        def _():
            w_arrive(1)

        @pl.when((i == 2) & mid)
        def _():
            w_arrive(2)

    third_sum(0)
    third_sum(1)
    chain(1, False)
    second(2)
    fold(3)

    @pl.when(edge)
    def _():
        w_arrive(1)

    @pl.when(mid)
    def _():
        w_arrive(3)

    qb_buf[t] = q_ref[pl.ds(pl.multiple_of(t * WINDOW, WINDOW), WINDOW), :]

    lanes = lax.broadcasted_iota(jnp.int32, (WINDOW, 128), 1)
    low = lanes < HEAD_DIM

    def doubled(part, rows, out):
        wide = rows.astype(jnp.float32)
        turned = pltpu.roll(wide, HEAD_DIM, 1)
        place = pl.ds(part * WINDOW, WINDOW)
        out[0, place, :] = jnp.where(low, wide, turned).astype(jnp.bfloat16)
        out[1, place, :] = jnp.where(low, turned, wide).astype(jnp.bfloat16)

    for i, (source, out) in enumerate(((key_ref, kdup), (value_ref, vdup))):
        doubled(1, source[pl.ds(pl.multiple_of(t * WINDOW, WINDOW), WINDOW), :], out)

        @pl.when(t > 0)
        def _():
            before = jnp.maximum(t - 1, 0) * WINDOW
            doubled(0, source[pl.ds(pl.multiple_of(before, WINDOW), WINDOW), :], out)

        @pl.when(takes)
        def _():
            if i == 0:
                received(halo, halo_rs.at[0])
            doubled(0, halo[i], out)

        @pl.when(me == 0)
        def _():
            doubled(0, jnp.zeros((WINDOW, 128), jnp.bfloat16), out)

    query_pos = lax.broadcasted_iota(jnp.int32, (WINDOW, 2 * WINDOW), 0) + WINDOW
    key_pos = lax.broadcasted_iota(jnp.int32, (WINDOW, 2 * WINDOW), 1)
    first = jnp.where(me == 0, WINDOW, 0)
    allowed = (key_pos <= query_pos) & (key_pos > query_pos - WINDOW) & (key_pos >= first)

    @jax.named_scope("attend")
    def attend_plane(i):
        zz = plane(i)
        if i == 0:
            received(qb_buf.at[0], q_rs.at[zz])
        else:
            received(qb_buf.at[0:2], q_rs.at[zz])

        @pl.loop(0, 2)
        def _(core):
            j = zz * 2 + core
            pair = qb_buf[j]
            kept = lax.div(j * KV_HEADS, ranks)
            keys, vals = kdup[kept], vdup[kept]
            line = l_buf[zz, e, core, e]
            outs = []
            for i in range(2):
                mine_half = low if i == 0 else jnp.logical_not(low)
                query = jnp.where(mine_half, pair, jnp.zeros_like(pair))
                scores = lax.dot_general(
                    query, keys, (((1,), (1,)), ((), ())), preferred_element_type=jnp.float32
                ) * HEAD_DIM ** (-0.5)
                masked = jnp.where(allowed, scores, big_negative)
                sink = line[:, row_count + i : row_count + i + 1]
                row_max = jnp.maximum(jnp.max(masked, -1, keepdims=True), sink)
                powers = jnp.exp(masked - row_max)
                totals = jnp.sum(powers, -1, keepdims=True) + jnp.exp(sink - row_max)
                probs = (powers / totals).astype(jnp.bfloat16)
                outs.append(jnp.dot(probs, vals, preferred_element_type=jnp.float32))
            att[:, pl.ds(pl.multiple_of(j * 128, 128), 128)] = jnp.where(low, outs[0], outs[1]).astype(
                jnp.bfloat16
            )

    attend_plane(0)
    third_sum(2)

    @pl.when(edge)
    def _():
        chain(2, False)

    second(3)
    attend_plane(1)

    @pl.when(mid)
    def _():
        chain(2, True)

    third_sum(3)

    @pl.when(edge)
    def _():
        chain(3, False)
        w_arrive(2)

    attend_plane(2)

    @pl.when(mid)
    def _():
        chain(3, True)

    attend_plane(3)

    @pl.when(edge)
    def _():
        w_arrive(3)

    with jax.named_scope("wwait"):
        for i in range(1, chips):
            zz = plane(i)
            received(w_buf.at[zz * 2 + c, taken, :], wx_rs.at[zz])
            w_rest(zz)
        received(w_buf.at[0:chips, other_carried, :], wp_rs.at[0])
        received(w_buf.at[0:chips, other_taken, :], wq_rs.at[0])
    with jax.named_scope("mix"):
        mix_v[...] = jnp.dot(
            att[...], w_buf[...].reshape(ranks * 128, width), preferred_element_type=jnp.float32
        ).astype(jnp.bfloat16)
    mix_out = pltpu.make_async_copy(mix_v, mix_hbm, out_sem.at[0])
    mix_out.start()

    for slot in (2, 3):
        for h in range(2):
            part = half(rc_buf.at[slot], h)
            with jax.named_scope("last"):
                received(part, rc_rs.at[slot * 2 + h])
                add_in(half(p_buf.at[z, e, c], h), part)

    moe_out = pltpu.make_async_copy(p_buf.at[z, e, c], moe_hbm, out_sem.at[1])
    moe_out.start()

    sent(r1_buf.at[0], x1_ss)
    sent(r1_buf.at[0:2], x2_ss)
    sent(r1_buf, pa_ss)
    sent(l_buf.at[0, :, 0], l1_ss)
    sent(l_buf.at[0], l2_ss)
    sent(l_buf.at[0:2], lp_ss)
    heavy, light = pl.ds(0, 3 * third), pl.ds(0, third)

    @pl.when(edge)
    def _():
        sent(x_buf.at[0, 0, 0], zo_ss)
        sent(l_buf.at[0, 0, 0], zlo_ss)
        sent(w_buf.at[0, heavy, :], wo_ss)

    @pl.when(mid)
    def _():
        sent(x_buf.at[0, 0], zo_ss)
        sent(l_buf.at[0, 0], zlo_ss)
        sent(w_buf.at[0:2, heavy, :], wo_ss)
        sent(r1_buf.at[0, 0:3], zf_ss)
        sent(l_buf.at[0, 0:3, 0], zlf_ss)
        sent(w_buf.at[0:3, heavy, :], wf_ss)

    sent(w_buf.at[0:chips, heavy, :], wp_ss)
    sent(w_buf.at[0:chips, light, :], wq_ss)
    sent(w_buf.at[0 : chips - 1, light, :], wx_ss)
    sent(r1_buf, s1_ss)
    sent(r1_buf.at[0:2], s2_ss)
    sent(r1_buf.at[0], s3_ss)
    sent(r1_buf.at[0, 0:3], rc_ss)
    sent(qb_buf.at[0 : ranks - 1], q_ss)

    @pl.when(gives)
    def _():
        sent(halo, halo_ss)

    with jax.named_scope("outs"):
        mix_out.wait()
        moe_out.wait()


def fused(
    queries,
    key_rows,
    value_rows,
    sink_logits,
    out_weight,
    moe_rows,
    moe_gain,
    routes,
    route_weight,
    gate_weight,
    up_weight,
    down_weight,
):
    groups, ranks = lax.axis_size("ep"), lax.axis_size("tp")
    chips = ranks // 2
    row_count, width = moe_rows.shape
    units = gate_weight.shape[2]
    bf16, f32 = jnp.bfloat16, jnp.float32
    vmem = pltpu.VMEM
    dma = pltpu.SemaphoreType.DMA
    one, two = chips, 2 * chips
    counts = (7, 2, 21, two, one, two, one, one, one, two, one)
    counts += (one, 1, one, 1, one, two, one, 8, one, 1)
    block = (row_count, width)
    in_vmem = pl.BlockSpec(memory_space=pltpu.VMEM)
    in_any = pl.BlockSpec(memory_space=pl.ANY)
    return pl.pallas_call(
        functools.partial(fused_kernel, groups, ranks),
        out_shape=(
            jax.ShapeDtypeStruct((queries.shape[0] // ranks, width), bf16),
            jax.ShapeDtypeStruct(block, bf16),
        ),
        in_specs=[in_vmem] * 5 + [in_any] * 7,
        out_specs=(in_any, in_any),
        scratch_shapes=[
            vmem((chips, groups, 2) + block, bf16),
            vmem((chips, groups, 2) + block, bf16),
            vmem((chips, groups) + block, bf16),
            vmem((2, chips) + block, bf16),
            vmem((chips,) + block, bf16),
            vmem((4,) + block, bf16),
            vmem((ranks,) + out_weight.shape, bf16),
            vmem((ranks, WINDOW, 128), bf16),
            vmem((chips, groups, 2, groups, 1, 128), f32),
            vmem((2, WINDOW, 128), bf16),
            vmem((2, 2 * WINDOW, 128), bf16),
            vmem((2, 2 * WINDOW, 128), bf16),
            vmem((WINDOW, ranks * 128), bf16),
            vmem((groups * 2 * row_count, units), bf16),
            vmem((queries.shape[0] // ranks, width), bf16),
            vmem(queries.shape, bf16),
            vmem(key_rows.shape, bf16),
            vmem(value_rows.shape, bf16),
            vmem((width, units), bf16),
            vmem((width, units), bf16),
            vmem((units, width), bf16),
        ]
        + [dma((count,)) for count in counts],
        compiler_params=pltpu.CompilerParams(
            collective_id=0, has_side_effects=True, vmem_limit_bytes=60 * 1024 * 1024
        ),
    )(
        routes.T,
        route_weight.T,
        sink_logits[None, :],
        moe_rows,
        moe_gain[None, :],
        queries,
        key_rows,
        value_rows,
        out_weight,
        gate_weight,
        up_weight,
        down_weight,
    )


def body(
    queries,
    key_rows,
    value_rows,
    sink_logits,
    out_weight,
    moe_rows,
    moe_gain,
    routes,
    route_weight,
    gate_weight,
    up_weight,
    down_weight,
):
    groups, ranks = lax.axis_size("ep"), lax.axis_size("tp")
    fits = groups == 4 and ranks == 8 and sink_logits.shape[0] == 2
    fits = fits and queries.shape == (ranks * WINDOW, 2 * HEAD_DIM)
    fits = fits and key_rows.shape[1] == 128 and moe_rows.shape[0] in (32, 64)
    if fits:
        return fused(
            queries,
            key_rows,
            value_rows,
            sink_logits,
            out_weight,
            moe_rows,
            moe_gain,
            routes,
            route_weight,
            gate_weight,
            up_weight,
            down_weight,
        )
    mixer_out = mixer(queries, key_rows, value_rows, sink_logits, out_weight)
    moe_out = experts(moe_rows, moe_gain, routes, route_weight, gate_weight, up_weight, down_weight)
    return (mixer_out, moe_out)


def solution(mesh):
    in_specs = (
        P("ep", "tp"),
        P("ep", None),
        P("ep", None),
        P("tp"),
        P("tp", None),
        P(("ep", "tp"), None),
        P(),
        P(("ep", "tp"), None),
        P(("ep", "tp"), None),
        P("ep", None, "tp"),
        P("ep", None, "tp"),
        P("ep", "tp", None),
    )
    out_specs = (P(("ep", "tp"), None), P(("ep", "tp"), None))
    return jax.shard_map(body, mesh=mesh, in_specs=in_specs, out_specs=out_specs, check_vma=False)
```

```python
import functools

import jax
import jax.numpy as jnp
from jax import lax
from jax.experimental import pallas as pl
from jax.experimental.pallas import tpu as pltpu
from jax.sharding import PartitionSpec as P

MESH = pl.DeviceIdType.MESH

HEADS = 16
KV_HEADS = 2
HEAD_DIM = 64
WINDOW = 128
TOP = 2


big_negative = -1e30
norm_eps = 1e-05
SHARE = 2


def passed_along(value, axis, steps):
    count = lax.axis_size(axis)
    initial, last = (max(0, -steps), min(count, count - steps))
    return lax.ppermute(value, axis, [(source, source + steps) for source in range(initial, last)])


def layer_normed(inputs, gain):
    values = inputs.astype(jnp.float32)
    center = values - jnp.mean(values, -1, keepdims=True)
    spread = jnp.mean(center * center, -1, keepdims=True)
    return (center * lax.rsqrt(spread + norm_eps) * gain).astype(jnp.bfloat16)


def attend(queries, key_rows, value_rows, sink_logits):
    total = queries.shape[0]
    heads_here = sink_logits.shape[0]
    blocks = total // WINDOW
    key_head = lax.axis_index("tp") * heads_here // (HEADS // KV_HEADS)
    key_own = lax.dynamic_slice_in_dim(key_rows, key_head * HEAD_DIM, HEAD_DIM, 1)
    value_own = lax.dynamic_slice_in_dim(value_rows, key_head * HEAD_DIM, HEAD_DIM, 1)
    last_rows = jnp.concatenate([key_own[total - WINDOW :], value_own[total - WINDOW :]], 1)
    earlier = passed_along(last_rows, "ep", 1)
    key_ext = jnp.concatenate([earlier[:, :HEAD_DIM], key_own], 0)
    value_ext = jnp.concatenate([earlier[:, HEAD_DIM:], value_own], 0)
    key_blocks = jnp.concatenate(
        [
            key_ext[:total].reshape(blocks, WINDOW, HEAD_DIM),
            key_ext[WINDOW:].reshape(blocks, WINDOW, HEAD_DIM),
        ],
        1,
    )
    value_blocks = jnp.concatenate(
        [
            value_ext[:total].reshape(blocks, WINDOW, HEAD_DIM),
            value_ext[WINDOW:].reshape(blocks, WINDOW, HEAD_DIM),
        ],
        1,
    )
    query_blocks = queries.reshape(blocks, WINDOW, heads_here, HEAD_DIM)
    scores = jnp.einsum(
        "nqhd,nkd->nhqk", query_blocks, key_blocks, preferred_element_type=jnp.float32
    ) * HEAD_DIM ** (-0.5)
    anchor = lax.axis_index("ep") * total
    block_base = anchor + jnp.arange(blocks, dtype=jnp.int32)[:, None, None] * WINDOW
    query_pos = block_base + jnp.arange(WINDOW, dtype=jnp.int32)[None, :, None]
    key_pos = block_base - WINDOW + jnp.arange(2 * WINDOW, dtype=jnp.int32)[None, None, :]
    allowed = ((key_pos <= query_pos) & (key_pos > query_pos - WINDOW) & (key_pos >= 0))[:, None]
    masked = jnp.where(allowed, scores, big_negative)
    sinks = sink_logits[None, :, None]
    row_max = jnp.maximum(jnp.max(masked, -1), sinks)
    powers = jnp.where(allowed, jnp.exp(masked - row_max[..., None]), 0.0)
    totals = jnp.sum(powers, -1) + jnp.exp(sinks - row_max)
    attn_probs = (powers / totals[..., None]).astype(jnp.bfloat16)
    attended = jnp.einsum(
        "nhqk,nkd->nqhd", attn_probs, value_blocks, preferred_element_type=jnp.float32
    )
    return attended.astype(jnp.bfloat16).reshape(total, heads_here * HEAD_DIM)


def mixer(queries, key_rows, value_rows, sink_logits, out_weight):
    attended = attend(queries, key_rows, value_rows, sink_logits)
    return lax.psum_scatter(
        jnp.dot(attended, out_weight, preferred_element_type=jnp.float32).astype(jnp.bfloat16),
        "tp",
        scatter_dimension=0,
        tiled=True,
    )


def experts(moe_rows, moe_gain, routes, route_weight, gate_weight, up_weight, down_weight):
    row_count = moe_rows.shape[0]
    width_all = moe_rows.shape[1]
    expert_count = gate_weight.shape[0] * lax.axis_size("ep")
    capacity = 3 * row_count * TOP // (2 * expert_count)
    normed = layer_normed(moe_rows, moe_gain)
    chosen = routes.reshape(-1)
    onehot = (chosen[:, None] == jnp.arange(expert_count, dtype=jnp.int32)[None, :]).astype(
        jnp.int32
    )
    earlier_count = jnp.cumsum(onehot, 0) - onehot
    slot_index = jnp.sum(earlier_count * onehot, 1)
    target = chosen * capacity + slot_index
    matches = target[None, :] == jnp.arange(expert_count * capacity, dtype=jnp.int32)[:, None]
    dispatch_map = jnp.sum(matches.reshape(expert_count * capacity, row_count, TOP), -1).astype(
        jnp.bfloat16
    )
    buffer = jnp.dot(dispatch_map, normed, preferred_element_type=jnp.float32).astype(jnp.bfloat16)
    buffer = buffer.reshape(expert_count, capacity, width_all)
    gate_mat = gate_weight[0]
    up_mat = up_weight[0]
    down_mat = down_weight[0]
    received = lax.all_to_all(buffer, "ep", split_axis=0, concat_axis=0, tiled=True)
    total = received.shape[0] * received.shape[1]
    flat_rows = received.reshape(total, width_all)
    shard_rows = lax.all_gather(flat_rows, "tp", axis=0, tiled=True)
    gate_val = jnp.dot(shard_rows, gate_mat, preferred_element_type=jnp.float32)
    up_val = jnp.dot(shard_rows, up_mat, preferred_element_type=jnp.float32)
    hidden = (jax.nn.silu(gate_val) * up_val).astype(jnp.bfloat16)
    summed = lax.psum_scatter(
        jnp.dot(hidden, down_mat, preferred_element_type=jnp.float32).astype(jnp.bfloat16),
        "tp",
        scatter_dimension=0,
        tiled=True,
    )
    results = summed.reshape(received.shape)
    returned = lax.all_to_all(results, "ep", split_axis=0, concat_axis=0, tiled=True)
    weights_flat = route_weight.reshape(-1)
    combine_map = jnp.sum(
        jnp.where(matches, weights_flat[None, :], 0.0).reshape(
            expert_count * capacity, row_count, TOP
        ),
        -1,
    )
    returned_flat = returned.reshape(expert_count * capacity, width_all).astype(jnp.float32)
    moe_out = lax.dot_general(
        combine_map, returned_flat, (((0,), (0,)), ((), ())), precision=lax.Precision.HIGHEST
    )
    return moe_out.astype(jnp.bfloat16)


def fused_kernel(
    groups,
    ranks,
    chosen_ref,
    weights_ref,
    sink_ref,
    rows_ref,
    gain_ref,
    q_hbm,
    key_hbm,
    value_hbm,
    ow_hbm,
    gate_hbm,
    up_hbm,
    down_hbm,
    mix_ref,
    moe_ref,
    x_buf,
    p_buf,
    r1_buf,
    r2_buf,
    r3_buf,
    rc_buf,
    w_buf,
    qb_buf,
    l_buf,
    halo,
    kdup,
    vdup,
    att,
    hid,
    q_ref,
    key_ref,
    value_ref,
    gate_w,
    up_w,
    down_w,
    load_sem,
    sem,
    z_rs,
    x1_rs,
    x2_rs,
    pa_rs,
    zl_rs,
    l1_rs,
    l2_rs,
    lp_rs,
    w_rs,
    wp_rs,
    wx_rs,
    wq_rs,
    s1_rs,
    s2_rs,
    s3_rs,
    rc_rs,
    q_rs,
    halo_rs,
):
    chips = ranks // 2
    e, t = lax.axis_index("ep"), lax.axis_index("tp")
    z, c = lax.div(t, 2), lax.rem(t, 2)
    y, x = lax.div(e, 2), lax.rem(e, 2)
    me = e * ranks + t
    ex, ey, e3 = e + 1 - 2 * x, e + 2 - 4 * y, 3 - e
    e1 = ex * (1 - c) + ey * c
    e2 = ey * (1 - c) + ex * c
    other = t + 1 - 2 * c
    oc = 1 - c
    mid = (z > 0) & (z < chips - 1)
    edge = jnp.logical_not(mid)
    row_count, width = rows_ref.shape
    half_rows = row_count // 2
    units = gate_w.shape[1]
    upper = lax.div(z, 2)
    order = (z, z + 1 - 2 * lax.rem(z, 2), 2 - upper, 3 * (1 - upper))

    def plane(i):
        if isinstance(i, int):
            return order[i]
        later = jnp.where(i == 2, order[2], order[3])
        return jnp.where(i == 0, order[0], jnp.where(i == 1, order[1], later))

    def from_above(zz):
        return jnp.where(zz > z, 1, 0)

    def remote(src, dst, ss, rs, to):
        return pltpu.make_async_remote_copy(
            src_ref=src, dst_ref=dst, send_sem=ss, recv_sem=rs, device_id=to, device_id_type=MESH
        )

    ss = [sem.at[k] for k in range(sem.shape[0])]
    (zo_ss, zf_ss, x1_ss, x2_ss, pa_ss, zlo_ss, zlf_ss, l1_ss, l2_ss, lp_ss) = ss[:10]
    (wo_ss, wf_ss, wp_ss, wx_ss, wq_ss, s1_ss, s2_ss, s3_ss, rc_ss, q_ss, halo_ss) = ss[10:]

    def received(dst, rs):
        remote(dst, dst, x1_ss, rs, (e, other)).wait_recv()

    def sent(src, send_sem):
        remote(src, src, send_sem, x1_rs.at[0], (e, other)).wait_send()

    loads = [
        pltpu.make_async_copy(ow_hbm, w_buf.at[t], load_sem.at[0]),
        pltpu.make_async_copy(key_hbm, key_ref, load_sem.at[1]),
        pltpu.make_async_copy(value_hbm, value_ref, load_sem.at[2]),
        pltpu.make_async_copy(q_hbm, q_ref, load_sem.at[3]),
        pltpu.make_async_copy(gate_hbm.at[0], gate_w, load_sem.at[4]),
        pltpu.make_async_copy(up_hbm.at[0], up_w, load_sem.at[5]),
        pltpu.make_async_copy(down_hbm.at[0], down_w, load_sem.at[6]),
    ]
    for load in loads:
        load.start()

    barrier = pltpu.get_barrier_semaphore()

    def greet(to):
        pl.semaphore_signal(barrier, inc=1, device_id=to, device_id_type=MESH)

    for to in ((e, other), (e1, t), (e2, t)):
        greet(to)

    @pl.when(z > 0)
    def _():
        greet((e, t - 2))

    @pl.when(z < chips - 1)
    def _():
        greet((e, t + 2))

    values = rows_ref[...].astype(jnp.float32)
    center = values - jnp.mean(values, -1, keepdims=True)
    spread_of = jnp.mean(center * center, -1, keepdims=True)
    x_buf[z, e, c] = (center * lax.rsqrt(spread_of + norm_eps) * gain_ref[...]).astype(jnp.bfloat16)
    lane = lax.broadcasted_iota(jnp.int32, (1, 128), 1)
    sinks = jnp.zeros((1, 128), jnp.float32)
    for i in range(2):
        sinks = jnp.where(lane == row_count + i, sink_ref[:, i : i + 1], sinks)
    chosen, weights = chosen_ref[...], weights_ref[...]
    for k in range(groups):
        named = jnp.where(chosen == k, weights, 0.0)
        l_buf[z, e, c, k] = sinks
        l_buf[z, e, c, k, :, 0:row_count] = jnp.sum(named, 0, keepdims=True)

    with jax.named_scope("barrier"):
        pl.semaphore_wait(barrier, jnp.where(mid, 5, 4))

    def half(block, h):
        return block.at[pl.ds(h * half_rows, half_rows), :]

    def pair_send(zz, column, x_sems, l_sems, to):
        for buf, (send_sem, recv_sem) in ((x_buf, x_sems), (l_buf, l_sems)):
            piece = buf.at[zz, column, c]
            remote(piece, piece, send_sem, recv_sem, to).start()

    def z_send(zz, to, h, send_sem, line_sem):
        part = half(x_buf.at[zz, e, c], h)
        remote(part, part, send_sem, z_rs.at[zz * 2 + h], to).start()
        if h == 1:
            line = l_buf.at[zz, e, c]
            remote(line, line, line_sem, zl_rs.at[zz], to).start()

    def spread(zz):
        for h in range(2):
            part = half(x_buf.at[zz, e, c], h)
            remote(part, part, x1_ss, x1_rs.at[zz * 2 + h], (e1, t)).start()
        line = l_buf.at[zz, e, c]
        remote(line, line, l1_ss, l1_rs.at[zz], (e1, t)).start()
        pair_send(zz, e, (x2_ss, x2_rs.at[zz]), (l2_ss, l2_rs.at[zz]), (e2, t))
        pair_send(zz, e, (pa_ss, pa_rs.at[zz]), (lp_ss, lp_rs.at[zz]), (e, other))

    def arrive_half(i, h):
        zz = plane(i)
        with jax.named_scope("half%d" % h):
            received(half(x_buf.at[zz, e, c], h), z_rs.at[zz * 2 + h])
        if h == 1:
            received(l_buf.at[zz, e, c], zl_rs.at[zz])

        @pl.when(mid)
        def _():
            z_send(zz, (e, t + 2 - 4 * from_above(zz)), h, zf_ss, zlf_ss)

    @jax.named_scope("arrive")
    def arrive(i):
        for h in range(2):
            arrive_half(i, h)

    @jax.named_scope("from_first")
    def from_first(zz):
        slot = chips + zz
        for h in range(2):
            part = half(x_buf.at[zz, e1, c], h)
            received(part, x1_rs.at[zz * 2 + h])
            remote(part, part, x2_ss, x2_rs.at[slot], (e2, t)).start()
        received(l_buf.at[zz, e1, c], l1_rs.at[zz])
        line = l_buf.at[zz, e1, c]
        remote(line, line, l2_ss, l2_rs.at[slot], (e2, t)).start()
        pair_send(zz, e1, (pa_ss, pa_rs.at[zz]), (lp_ss, lp_rs.at[zz]), (e, other))

    @jax.named_scope("from_second")
    def from_second(zz):
        for slot, column in ((0, e2), (1, e3)):
            where = slot * chips + zz
            received(x_buf.at[zz, column, c], x2_rs.at[where])
            received(l_buf.at[zz, column, c], l2_rs.at[where])
            pair_send(zz, column, (pa_ss, pa_rs.at[zz]), (lp_ss, lp_rs.at[zz]), (e, other))

    @jax.named_scope("from_partner")
    def from_partner(zz):
        received(x_buf.at[zz, :, oc], pa_rs.at[zz])
        received(l_buf.at[zz, :, oc], lp_rs.at[zz])

    all_rows = w_buf.shape[1]
    fewer = all_rows * SHARE // 8
    more = all_rows - fewer
    side = x * (1 - c) + y * c
    other_side = x * c + y * (1 - c)

    def span(which, step, size):
        return pl.ds(pl.multiple_of(which * step, 16), size)

    carried, given = span(side, fewer, more), span(side, more, fewer)
    taken = span(1 - side, more, fewer)
    other_carried, other_taken = span(other_side, fewer, more), span(1 - other_side, more, fewer)

    def w_send(zz, to, send_sem):
        block = w_buf.at[zz * 2 + c, carried, :]
        remote(block, block, send_sem, w_rs.at[zz], to).start()

    def w_partner(zz):
        block = w_buf.at[zz * 2 + c, carried, :]
        remote(block, block, wp_ss, wp_rs.at[0], (e, other)).start()

    def w_rest(zz):
        rest = w_buf.at[zz * 2 + c, taken, :]
        remote(rest, rest, wq_ss, wq_rs.at[0], (e, other)).start()

    @jax.named_scope("w_arrive")
    def w_arrive(i):
        zz = plane(i)
        received(w_buf.at[zz * 2 + c, carried, :], w_rs.at[zz])

        @pl.when(mid)
        def _():
            w_send(zz, (e, t + 2 - 4 * from_above(zz)), wf_ss)

        piece = w_buf.at[zz * 2 + c, given, :]
        remote(piece, piece, wx_ss, wx_rs.at[zz], (e1, t)).start()
        w_partner(zz)

    def q_send(zz):
        for core in range(2):
            tt = zz * 2 + core

            @pl.when(tt != t)
            def _():
                remote(
                    q_ref.at[pl.ds(pl.multiple_of(tt * WINDOW, WINDOW), WINDOW), :],
                    qb_buf.at[t],
                    q_ss,
                    q_rs.at[z],
                    (e, tt),
                ).start()

    for h in range(2):

        @pl.when(z < chips - 1)
        def _():
            z_send(z, (e, t + 2), h, zo_ss, zlo_ss)

        @pl.when(z > 0)
        def _():
            z_send(z, (e, t - 2), h, zo_ss, zlo_ss)

    spread(z)
    loads[0].wait()
    toward = t - 2 + 4 * from_above(plane(1))

    @pl.when(edge)
    def _():
        w_send(z, (e, toward), wo_ss)

    w_partner(z)
    w_rest(z)

    @pl.when(mid)
    def _():
        for h in range(2):
            arrive_half(1, h)
            arrive_half(2, h)
        w_send(z, (e, 2 * t - toward), wo_ss)

    pl.when(edge)(functools.partial(arrive, 1))
    from_first(z)
    spread(plane(1))
    pl.when(edge)(functools.partial(arrive, 2))
    spread(plane(2))

    @pl.when(mid)
    def _():
        arrive(3)
        w_send(z, (e, toward), wo_ss)

    from_second(z)

    @pl.when(mid)
    def _():
        from_first(plane(1))
        spread(plane(3))

    from_partner(z)
    for load in loads[1:4]:
        load.wait()

    last = key_ref.shape[0] - WINDOW
    gives = (t == 0) & (e < groups - 1)
    takes = (t == 0) & (e > 0)
    for i, source in enumerate((key_ref, value_ref)):
        copy = remote(
            source.at[pl.ds(last, WINDOW), :],
            halo.at[i],
            halo_ss,
            halo_rs.at[0],
            (lax.rem(e + 1, groups), t),
        )
        pl.when(gives)(copy.start)

    q_send(z)
    for load in loads[4:6]:
        load.wait()

    diagonal = lax.broadcasted_iota(jnp.int32, (row_count, 128), 0) == lax.broadcasted_iota(
        jnp.int32, (row_count, 128), 1
    )
    cut = (-(-units // 256) + 1) // 2 * 256
    rows_in_plane = groups * 2 * row_count

    @jax.named_scope("gate_up")
    def gate_up(zz, begin, end):
        rows = x_buf[zz].reshape(rows_in_plane, width)
        gate_val = jnp.dot(rows, gate_w[:, begin:end], preferred_element_type=jnp.float32)
        up_val = jnp.dot(rows, up_w[:, begin:end], preferred_element_type=jnp.float32)
        hid[:, begin:end] = (gate_val / (1.0 + jnp.exp(-gate_val)) * up_val).astype(jnp.bfloat16)

    def add_in(block, extra):
        block[...] = (block[...].astype(jnp.float32) + extra[...].astype(jnp.float32)).astype(
            jnp.bfloat16
        )

    @jax.named_scope("fold")
    def fold(i):
        zz = plane(i)
        received(r1_buf.at[zz], s1_rs.at[zz])
        for n, column in enumerate((e3, e2, e1, e)):
            block = p_buf.at[zz, column, c]
            add_in(block, r1_buf.at[zz, column])
            if n == 0:
                for h in range(2):
                    part, into = half(block, h), half(r2_buf.at[1, zz], h)
                    remote(part, into, s2_ss, s2_rs.at[chips + zz * 2 + h], (e2, t)).start()
            if n == 1:
                remote(block, r2_buf.at[0, zz], s2_ss, s2_rs.at[zz], (e2, t)).start()

    @jax.named_scope("second")
    def second(i):
        zz = plane(i)
        for h in range(2):
            extra, part = half(r2_buf.at[1, zz], h), half(p_buf.at[zz, e1, c], h)
            received(extra, s2_rs.at[chips + zz * 2 + h])
            add_in(part, extra)
            into = half(r3_buf.at[zz], h)
            remote(part, into, s3_ss, s3_rs.at[zz * 2 + h], (e1, t)).start()

    @jax.named_scope("third_sum")
    def third_half(i, h):
        zz = plane(i)
        if h == 0:
            received(r2_buf.at[0, zz], s2_rs.at[zz])
        received(half(r3_buf.at[zz], h), s3_rs.at[zz * 2 + h])
        part = half(p_buf.at[zz, e, c], h)
        part[...] = (
            part[...].astype(jnp.float32)
            + half(r2_buf.at[0, zz], h)[...].astype(jnp.float32)
            + half(r3_buf.at[zz], h)[...].astype(jnp.float32)
        ).astype(jnp.bfloat16)

    def chain_half(i, h, passing):
        zz = plane(i)
        hops = 2 if passing and i == 3 else 1
        to = (e, t + hops * (4 * from_above(zz) - 2))
        slot = 2 if i == 1 else 3 if passing else i - 2
        part = half(p_buf.at[zz, e, c], h)
        if passing:
            extra = half(rc_buf.at[i - 2], h)
            received(extra, rc_rs.at[(i - 2) * 2 + h])
            add_in(part, extra)
        remote(part, half(rc_buf.at[slot], h), rc_ss, rc_rs.at[slot * 2 + h], to).start()

    def third_sum(i):
        for h in range(2):
            third_half(i, h)
            if i == 1:
                chain_half(i, h, False)
            if i > 1:
                pl.when(edge)(functools.partial(chain_half, i, h, False))

    @jax.named_scope("chain")
    def chain(i):
        for h in range(2):
            chain_half(i, h, True)

    @pl.loop(0, groups)
    def _(i):
        zz = plane(i)

        @pl.when(i > 0)
        def _():
            from_partner(zz)
            q_send(zz)

        gate_up(zz, 0, cut)

        @pl.when((i == 0) & edge)
        def _():
            from_first(plane(1))

        @pl.when((i == 1) & mid)
        def _():
            from_first(plane(3))
            w_arrive(2)

        @pl.when(i == 2)
        def _():
            fold(1)

        @pl.when(i == 3)
        def _():
            fold(2)

        gate_up(zz, cut, units)

        @pl.when(i == 0)
        def _():
            loads[6].wait()

        @pl.when((i == 1) & mid)
        def _():
            fold(0)
            from_second(plane(2))

        @pl.when(i == 2)
        def _():
            from_second(plane(3))
            pl.when(mid)(functools.partial(w_arrive, 3))

        @pl.when(i == 3)
        def _():
            second(1)

        shares = []
        for column in range(groups):
            for core in range(2):
                line = l_buf[zz, column, core, e]
                shares.append(
                    jnp.sum(
                        jnp.where(diagonal, jnp.broadcast_to(line, (row_count, 128)), 0.0),
                        -1,
                        keepdims=True,
                    )
                )
        share = jnp.concatenate(shares, 0)
        with jax.named_scope("down"):
            down = jnp.dot(hid[...], down_w[...], preferred_element_type=jnp.float32)
            p_buf[zz] = (down * share).astype(jnp.bfloat16).reshape(groups, 2, row_count, width)
        remote(p_buf.at[zz, :, oc], r1_buf.at[zz], s1_ss, s1_rs.at[zz], (e, other)).start()

        @pl.when(i == 0)
        def _():
            from_first(plane(2))
            pl.when(mid)(functools.partial(w_arrive, 1))
            from_second(plane(1))

            @pl.when(edge)
            def _():
                arrive(3)
                spread(plane(3))

        @pl.when((i == 1) & edge)
        def _():
            from_second(plane(2))
            from_first(plane(3))
            fold(0)

        @pl.when(i == 2)
        def _():
            second(0)
            pl.when(edge)(functools.partial(w_arrive, 1))

    qb_buf[t] = q_ref[pl.ds(pl.multiple_of(t * WINDOW, WINDOW), WINDOW), :]

    lanes = lax.broadcasted_iota(jnp.int32, (WINDOW, 128), 1)
    low = lanes < HEAD_DIM

    def doubled(part, rows, out):
        wide = rows.astype(jnp.float32)
        turned = pltpu.roll(wide, HEAD_DIM, 1)
        place = pl.ds(part * WINDOW, WINDOW)
        out[0, place, :] = jnp.where(low, wide, turned).astype(jnp.bfloat16)
        out[1, place, :] = jnp.where(low, turned, wide).astype(jnp.bfloat16)

    for i, (source, out) in enumerate(((key_ref, kdup), (value_ref, vdup))):
        doubled(1, source[pl.ds(pl.multiple_of(t * WINDOW, WINDOW), WINDOW), :], out)

        @pl.when(t > 0)
        def _():
            before = jnp.maximum(t - 1, 0) * WINDOW
            doubled(0, source[pl.ds(pl.multiple_of(before, WINDOW), WINDOW), :], out)

        @pl.when(takes)
        def _():
            if i == 0:
                received(halo, halo_rs.at[0])
            doubled(0, halo[i], out)

        @pl.when(me == 0)
        def _():
            doubled(0, jnp.zeros((WINDOW, 128), jnp.bfloat16), out)

    query_pos = lax.broadcasted_iota(jnp.int32, (WINDOW, 2 * WINDOW), 0) + WINDOW
    key_pos = lax.broadcasted_iota(jnp.int32, (WINDOW, 2 * WINDOW), 1)
    first = jnp.where(me == 0, WINDOW, 0)
    allowed = (key_pos <= query_pos) & (key_pos > query_pos - WINDOW) & (key_pos >= first)

    def q_wait(i):
        if i == 0:
            received(qb_buf.at[0], q_rs.at[z])
        else:
            received(qb_buf.at[0:2], q_rs.at[plane(i)])

    @jax.named_scope("attend")
    def attend(begin, end):
        for n in range(begin, end):
            zz, core = plane(n // 2), n % 2
            j = zz * 2 + core
            pair = qb_buf[j] * jnp.asarray(HEAD_DIM ** (-0.5), jnp.bfloat16)
            kept = lax.div(j * KV_HEADS, ranks)
            keys, vals = kdup[kept], vdup[kept]
            line = l_buf[zz, e, core, e]
            outs = []
            for i in range(2):
                mine_half = low if i == 0 else jnp.logical_not(low)
                query = jnp.where(mine_half, pair, jnp.zeros_like(pair))
                scores = lax.dot_general(
                    query, keys, (((1,), (1,)), ((), ())), preferred_element_type=jnp.float32
                )
                masked = jnp.where(allowed, scores, big_negative)
                sink = line[:, row_count + i : row_count + i + 1]
                row_max = jnp.maximum(jnp.max(masked, -1, keepdims=True), sink)
                powers = jnp.exp(masked - row_max)
                totals = jnp.sum(powers, -1, keepdims=True) + jnp.exp(sink - row_max)
                probs = (powers * (1.0 / totals)).astype(jnp.bfloat16)
                outs.append(jnp.dot(probs, vals, preferred_element_type=jnp.float32))
            att[:, pl.ds(pl.multiple_of(j * 128, 128), 128)] = jnp.where(low, outs[0], outs[1]).astype(
                jnp.bfloat16
            )

    q_wait(0)
    attend(0, 1)
    fold(3)
    second(2)
    pl.when(edge)(functools.partial(w_arrive, 2))
    attend(1, 2)
    q_wait(1)
    attend(2, 4)
    third_sum(1)
    second(3)
    third_sum(2)
    pl.when(edge)(functools.partial(w_arrive, 3))
    q_wait(2)
    attend(4, 6)
    third_sum(3)
    pl.when(mid)(functools.partial(chain, 2))
    q_wait(3)
    attend(6, ranks)
    pl.when(mid)(functools.partial(chain, 3))
    third_sum(0)

    with jax.named_scope("wwait"):
        for i in range(1, chips):
            zz = plane(i)
            received(w_buf.at[zz * 2 + c, taken, :], wx_rs.at[zz])
            w_rest(zz)
        received(w_buf.at[0:chips, other_carried, :], wp_rs.at[0])
        received(w_buf.at[0:chips, other_taken, :], wq_rs.at[0])
    with jax.named_scope("mix"):
        mix_ref[...] = jnp.dot(
            att[...], w_buf[...].reshape(ranks * 128, width), preferred_element_type=jnp.float32
        ).astype(jnp.bfloat16)
    for h in range(2):
        with jax.named_scope("last"):
            total = half(p_buf.at[z, e, c], h)[...].astype(jnp.float32)
            for slot in (2, 3):
                part = half(rc_buf.at[slot], h)
                received(part, rc_rs.at[slot * 2 + h])
                total = total + part[...].astype(jnp.float32)
            half(moe_ref, h)[...] = total.astype(jnp.bfloat16)

    sent(r1_buf.at[0], x1_ss)
    sent(r1_buf.at[0:2], x2_ss)
    sent(r1_buf, pa_ss)
    sent(l_buf.at[0, :, 0], l1_ss)
    sent(l_buf.at[0], l2_ss)
    sent(l_buf.at[0:2], lp_ss)
    heavy, light = pl.ds(0, more), pl.ds(0, fewer)

    @pl.when(edge)
    def _():
        sent(x_buf.at[0, 0, 0], zo_ss)
        sent(l_buf.at[0, 0, 0], zlo_ss)
        sent(w_buf.at[0, heavy, :], wo_ss)

    @pl.when(mid)
    def _():
        sent(x_buf.at[0, 0], zo_ss)
        sent(l_buf.at[0, 0], zlo_ss)
        sent(w_buf.at[0:2, heavy, :], wo_ss)
        sent(r1_buf.at[0, 0:3], zf_ss)
        sent(l_buf.at[0, 0:3, 0], zlf_ss)
        sent(w_buf.at[0:3, heavy, :], wf_ss)


    sent(w_buf.at[0:chips, heavy, :], wp_ss)
    sent(w_buf.at[0:chips, light, :], wq_ss)
    sent(w_buf.at[0 : chips - 1, light, :], wx_ss)
    sent(r1_buf, s1_ss)
    sent(r1_buf.at[0:2], s2_ss)
    sent(r1_buf.at[0], s3_ss)
    sent(r1_buf.at[0, 0:3], rc_ss)
    sent(qb_buf.at[0 : ranks - 1], q_ss)

    @pl.when(gives)
    def _():
        sent(halo, halo_ss)


def fused(
    queries,
    key_rows,
    value_rows,
    sink_logits,
    out_weight,
    moe_rows,
    moe_gain,
    routes,
    route_weight,
    gate_weight,
    up_weight,
    down_weight,
):
    groups, ranks = lax.axis_size("ep"), lax.axis_size("tp")
    chips = ranks // 2
    row_count, width = moe_rows.shape
    units = gate_weight.shape[2]
    bf16, f32 = jnp.bfloat16, jnp.float32
    vmem = pltpu.VMEM
    dma = pltpu.SemaphoreType.DMA
    one, two = chips, 2 * chips
    counts = (7, 21, two, two, two, one, one, one, two, one)
    counts += (one, 1, one, 1, one, 3 * chips, two, 8, one, 1)
    block = (row_count, width)
    in_vmem = pl.BlockSpec(memory_space=pltpu.VMEM)
    in_any = pl.BlockSpec(memory_space=pl.ANY)
    return pl.pallas_call(
        functools.partial(fused_kernel, groups, ranks),
        out_shape=(
            pltpu.VMEM((queries.shape[0] // ranks, width), bf16),
            pltpu.VMEM(block, bf16),
        ),
        in_specs=[in_vmem] * 5 + [in_any] * 7,
        out_specs=(in_vmem, in_vmem),
        scratch_shapes=[
            vmem((chips, groups, 2) + block, bf16),
            vmem((chips, groups, 2) + block, bf16),
            vmem((chips, groups) + block, bf16),
            vmem((2, chips) + block, bf16),
            vmem((chips,) + block, bf16),
            vmem((4,) + block, bf16),
            vmem((ranks,) + out_weight.shape, bf16),
            vmem((ranks, WINDOW, 128), bf16),
            vmem((chips, groups, 2, groups, 1, 128), f32),
            vmem((2, WINDOW, 128), bf16),
            vmem((2, 2 * WINDOW, 128), bf16),
            vmem((2, 2 * WINDOW, 128), bf16),
            vmem((WINDOW, ranks * 128), bf16),
            vmem((groups * 2 * row_count, units), bf16),
            vmem(queries.shape, bf16),
            vmem(key_rows.shape, bf16),
            vmem(value_rows.shape, bf16),
            vmem((width, units), bf16),
            vmem((width, units), bf16),
            vmem((units, width), bf16),
        ]
        + [dma((count,)) for count in counts],
        compiler_params=pltpu.CompilerParams(
            collective_id=0, has_side_effects=True, vmem_limit_bytes=60 * 1024 * 1024
        ),
    )(
        routes.T,
        route_weight.T,
        sink_logits[None, :],
        moe_rows,
        moe_gain[None, :],
        queries,
        key_rows,
        value_rows,
        out_weight,
        gate_weight,
        up_weight,
        down_weight,
    )


def body(
    queries,
    key_rows,
    value_rows,
    sink_logits,
    out_weight,
    moe_rows,
    moe_gain,
    routes,
    route_weight,
    gate_weight,
    up_weight,
    down_weight,
):
    groups, ranks = lax.axis_size("ep"), lax.axis_size("tp")
    fits = groups == 4 and ranks == 8 and sink_logits.shape[0] == 2
    fits = fits and queries.shape == (ranks * WINDOW, 2 * HEAD_DIM)
    fits = fits and key_rows.shape[1] == 128 and moe_rows.shape[0] in (32, 64)
    if fits:
        return fused(
            queries,
            key_rows,
            value_rows,
            sink_logits,
            out_weight,
            moe_rows,
            moe_gain,
            routes,
            route_weight,
            gate_weight,
            up_weight,
            down_weight,
        )
    mixer_out = mixer(queries, key_rows, value_rows, sink_logits, out_weight)
    moe_out = experts(moe_rows, moe_gain, routes, route_weight, gate_weight, up_weight, down_weight)
    return (mixer_out, moe_out)


def solution(mesh):
    in_specs = (
        P("ep", "tp"),
        P("ep", None),
        P("ep", None),
        P("tp"),
        P("tp", None),
        P(("ep", "tp"), None),
        P(),
        P(("ep", "tp"), None),
        P(("ep", "tp"), None),
        P("ep", None, "tp"),
        P("ep", None, "tp"),
        P("ep", "tp", None),
    )
    out_specs = (P(("ep", "tp"), None), P(("ep", "tp"), None))
    return jax.shard_map(body, mesh=mesh, in_specs=in_specs, out_specs=out_specs, check_vma=False)
```
